32 devices in a mesh: fs: 8 (over z, core), tp: 4 (over y, x).
Axes of the slice: x: 2, y: 2, z: 4, core: 2. Of those that a mesh axis runs over, the one named last changes fastest.
Arguments:
- late_input: bfloat16 [1024, 2048], P('fs'), may hold values from -6 to 6
- early_input: bfloat16 [1024, 2048], P('fs'), may hold values from -6 to 6
- early_mid: bfloat16 [1024, 2048], P('fs'), may hold values from -6 to 6
- cotangent: bfloat16 [1024, 2048], P('fs'), may hold values from -6 to 6
- gain_first: float32 [2048], replicated, may hold values from 0.1 to 1.9
- gain_second: float32 [2048], replicated, may hold values from 0.1 to 1.9
- gate_first: bfloat16 [2048, 2816], P('fs', 'tp'), may hold values from -0.125 to 0.125
- up_first: bfloat16 [2048, 2816], P('fs', 'tp'), may hold values from -0.125 to 0.125
- down_first: bfloat16 [2816, 2048], P('tp', 'fs'), may hold values from -0.109375 to 0.109375
- gate_second: bfloat16 [2048, 2816], P('fs', 'tp'), may hold values from -0.125 to 0.125
- up_second: bfloat16 [2048, 2816], P('fs', 'tp'), may hold values from -0.125 to 0.125
- down_second: bfloat16 [2816, 2048], P('tp', 'fs'), may hold values from -0.109375 to 0.109375
- sum_gate_first: float32 [2048, 2816], P('fs', 'tp'), may hold values from -128 to 128
- sum_up_first: float32 [2048, 2816], P('fs', 'tp'), may hold values from -128 to 128
- sum_down_first: float32 [2816, 2048], P('tp', 'fs'), may hold values from -128 to 128
- sum_gate_second: float32 [2048, 2816], P('fs', 'tp'), may hold values from -128 to 128
- sum_up_second: float32 [2048, 2816], P('fs', 'tp'), may hold values from -128 to 128
- sum_down_second: float32 [2816, 2048], P('tp', 'fs'), may hold values from -128 to 128
Outputs:
- late_mid: bfloat16 [1024, 2048], P('fs')
- late_out: bfloat16 [1024, 2048], P('fs')
- input_grad: bfloat16 [1024, 2048], P('fs')
- new_gate_first: float32 [2048, 2816], P('fs', 'tp')
- new_up_first: float32 [2048, 2816], P('fs', 'tp')
- new_down_first: float32 [2816, 2048], P('tp', 'fs')
- new_gate_second: float32 [2048, 2816], P('fs', 'tp')
- new_up_second: float32 [2048, 2816], P('fs', 'tp')
- new_down_second: float32 [2816, 2048], P('tp', 'fs')
The draws below stay inside these ranges and needn't reach their ends.
All inputs are finite; a program needn't handle non-finite values.
Results may differ from the reference program's by a relative error of at most 0.015.
Values may be sent and summed in bfloat16 or wider, within the bound.
A program may use at most 128 MiB of HBM per device.

```python
import jax
import jax.numpy as jnp
from jax import lax

D = 2048
FF = 2816
TOKENS = 1024
N_TP = 4


def with_spikes(result, own_key, source, target, parts, factor):
    def block_of(dim):
        return (jnp.arange(result.shape[dim]) // (result.shape[dim] // parts)).reshape((-1,) + (1,) * (result.ndim - 1 - dim))

    near = jax.random.permutation(own_key, parts)[block_of(target)]
    other_side = (block_of(target) + parts // 2) % parts
    return jnp.where((block_of(source) == near) | (block_of(source) == other_side), factor * result, result)


def level_of(key, shape, shards, smallest, top_value):
    factor_of, own = 1.0, jax.random.fold_in(key, 6)
    for dim, shards_of in shards:
        steps = jnp.exp(jax.random.uniform(jax.random.fold_in(own, dim), (shards_of,), jnp.float32, smallest / len(shards), top_value / len(shards)))
        factor_of = factor_of * jnp.repeat(steps, shape[dim] // shards_of).reshape([-1 if axis == dim else 1 for axis in range(len(shape))])
    return factor_of


def bell_draw(own_key, dims, width, most, split=(), held_as=jnp.bfloat16):
    array = jax.random.normal(own_key, dims, jnp.float32) * width
    if len(split) > 0:
        array = level_of(own_key, dims, split, -0.22, 0.18) * array
    return jnp.clip(array, min=-most, max=most).astype(held_as)


def bell_draw_with(rng, dims, width, most, pieces, heavy, dtype=jnp.bfloat16):
    values = width * jax.random.normal(rng, dims, jnp.float32)
    if pieces:
        values = values * level_of(rng, dims, pieces, -0.22, 0.18)
    return jnp.clip(with_spikes(values, jax.random.fold_in(rng, 3), *heavy), -most, most).astype(dtype)


def setup_inputs(seed: int = 0) -> dict:
    streams_of = jax.random.split(jax.random.key(seed), 19)
    late_input = bell_draw(streams_of[0], (TOKENS, D), 1.0, 6.0, ((0, 8),))
    early_input = bell_draw(streams_of[1], (TOKENS, D), 1.0, 6.0, ((0, 8),))
    early_mid = bell_draw(streams_of[2], (TOKENS, D), 1.0, 6.0, ((0, 8),))
    cotangent = bell_draw_with(streams_of[3], (TOKENS, D), 1.0, 6.0, ((0, 8),), (0, 1, 8, 2.0))
    gain_first = jnp.clip(1.0 + 0.18 * jax.random.normal(streams_of[4], (D,), jnp.float32), 0.1, 1.9)
    gain_second = jnp.clip(1.0 + 0.18 * jax.random.normal(streams_of[5], (D,), jnp.float32), 0.1, 1.9)
    gate_first = bell_draw(streams_of[6], (D, FF), D ** -0.5, 0.125, ((0, 8), (1, 4)))
    up_first = bell_draw(streams_of[7], (D, FF), D ** -0.5, 0.125, ((0, 8), (1, 4)))
    down_first = bell_draw(streams_of[8], (FF, D), FF ** -0.5, 0.109375, ((0, 4), (1, 8)))
    gate_second = bell_draw(streams_of[9], (D, FF), D ** -0.5, 0.125, ((0, 8), (1, 4)))
    up_second = bell_draw(streams_of[10], (D, FF), D ** -0.5, 0.125, ((0, 8), (1, 4)))
    down_second = bell_draw(streams_of[11], (FF, D), FF ** -0.5, 0.109375, ((0, 4), (1, 8)))
    sum_gate_first = bell_draw(streams_of[12], (D, FF), (0.25 * TOKENS ** 0.5), 128.0, ((0, 8), (1, 4)), jnp.float32)
    sum_up_first = bell_draw(streams_of[13], (D, FF), (0.25 * TOKENS ** 0.5), 128.0, ((0, 8), (1, 4)), jnp.float32)
    sum_down_first = bell_draw(streams_of[14], (FF, D), (0.25 * TOKENS ** 0.5), 128.0, ((0, 4), (1, 8)), jnp.float32)
    sum_gate_second = bell_draw(streams_of[15], (D, FF), (0.25 * TOKENS ** 0.5), 128.0, ((0, 8), (1, 4)), jnp.float32)
    sum_up_second = bell_draw(streams_of[16], (D, FF), (0.25 * TOKENS ** 0.5), 128.0, ((0, 8), (1, 4)), jnp.float32)
    sum_down_second = bell_draw(streams_of[17], (FF, D), (0.25 * TOKENS ** 0.5), 128.0, ((0, 4), (1, 8)), jnp.float32)
    return {"late_input": late_input, "early_input": early_input, "early_mid": early_mid, "cotangent": cotangent, "gain_first": gain_first, "gain_second": gain_second, "gate_first": gate_first, "up_first": up_first, "down_first": down_first, "gate_second": gate_second, "up_second": up_second, "down_second": down_second, "sum_gate_first": sum_gate_first, "sum_up_first": sum_up_first, "sum_down_first": sum_down_first, "sum_gate_second": sum_gate_second, "sum_up_second": sum_up_second, "sum_down_second": sum_down_second}


norm_eps = 1e-06

def normalize(values, gain_vector):
    widened = values.astype(jnp.float32)
    factor = lax.rsqrt(lax.optimization_barrier(jnp.mean(widened * widened, axis=-1, keepdims=True)) + norm_eps)
    normed = (widened * factor * gain_vector.astype(jnp.float32)).astype(jnp.bfloat16)
    return (widened, factor, normed)

def groupwise(operands, part_count):
    part_width = operands[0][0].shape[1] // part_count
    running = jnp.zeros((operands[0][0].shape[0], operands[0][1].shape[1]), jnp.float32)
    for part_index in range(part_count):
        lower = part_index * part_width
        product = jnp.zeros_like(running)
        for left_rows, right_cols in operands:
            product = product + jnp.dot(left_rows[:, lower:lower + part_width], right_cols[lower:lower + part_width], preferred_element_type=jnp.float32)
        rounded = lax.optimization_barrier(product.astype(jnp.bfloat16))
        running = running + rounded.astype(jnp.float32)
    return running

def block_forward(values, gain_vector, w_gate, w_up, w_down):
    widened, factor, normed = normalize(values, gain_vector)
    gate_pre = jnp.dot(normed, w_gate, preferred_element_type=jnp.float32)
    up_pre = jnp.dot(normed, w_up, preferred_element_type=jnp.float32)
    hidden = (jax.nn.silu(gate_pre) * up_pre).astype(jnp.bfloat16)
    branch = groupwise(((hidden, w_down),), N_TP)
    return (widened + 0.5 * branch).astype(jnp.bfloat16)

def block_backward(values, cotangent, gain_vector, w_gate, w_up, w_down):
    widened, factor, normed = normalize(values, gain_vector)
    gate_pre = jnp.dot(normed, w_gate, preferred_element_type=jnp.float32)
    up_pre = jnp.dot(normed, w_up, preferred_element_type=jnp.float32)
    sigmoid_gate = jax.nn.sigmoid(gate_pre)
    activated = gate_pre * sigmoid_gate
    hidden = (activated * up_pre).astype(jnp.bfloat16)
    hidden_grad = 0.5 * jnp.dot(cotangent, w_down.T, preferred_element_type=jnp.float32)
    gate_grad = (hidden_grad * up_pre * sigmoid_gate * (1.0 + gate_pre * (1.0 - sigmoid_gate))).astype(jnp.bfloat16)
    up_grad = (hidden_grad * activated).astype(jnp.bfloat16)
    normed_grad = groupwise(((gate_grad, w_gate.T), (up_grad, w_up.T)), N_TP)
    scaled = normed_grad * gain_vector.astype(jnp.float32)
    unit_rows = widened * factor
    rows_grad = cotangent.astype(jnp.float32) + factor * (scaled - unit_rows * lax.optimization_barrier(jnp.mean(scaled * unit_rows, axis=-1, keepdims=True)))
    grad_gate = jnp.dot(normed.T, gate_grad, preferred_element_type=jnp.float32)
    grad_up = jnp.dot(normed.T, up_grad, preferred_element_type=jnp.float32)
    grad_down = 0.5 * jnp.dot(hidden.T, cotangent, preferred_element_type=jnp.float32)
    return (rows_grad, (grad_gate, grad_up, grad_down))

def reference(late_input, early_input, early_mid, cotangent, gain_first, gain_second, gate_first, up_first, down_first, gate_second, up_second, down_second, sum_gate_first, sum_up_first, sum_down_first, sum_gate_second, sum_up_second, sum_down_second):
    late_mid = block_forward(late_input, gain_first, gate_first, up_first, down_first)
    late_out = block_forward(late_mid, gain_second, gate_second, up_second, down_second)
    mid_grad, grads_second = block_backward(early_mid, cotangent, gain_second, gate_second, up_second, down_second)
    mid_grad = mid_grad.astype(jnp.bfloat16)
    rows_grad, grads_first = block_backward(early_input, mid_grad, gain_first, gate_first, up_first, down_first)
    return (late_mid, late_out, rows_grad.astype(jnp.bfloat16), sum_gate_first + grads_first[0], sum_up_first + grads_first[1], sum_down_first + grads_first[2], sum_gate_second + grads_second[0], sum_up_second + grads_second[1], sum_down_second + grads_second[2])
```

```python
import jax
import jax.numpy as jnp
from jax import lax
from jax.sharding import PartitionSpec as P

norm_eps = 1e-06


def normalize(values, gain_vector):
    widened = values.astype(jnp.float32)
    factor = lax.rsqrt(jnp.mean(widened * widened, axis=-1, keepdims=True) + norm_eps)
    normed = (widened * factor * gain_vector).astype(jnp.bfloat16)
    return (widened, factor, normed)


def project(rows, weights):
    return jnp.dot(rows, weights, preferred_element_type=jnp.float32)


def project_back(hidden_rows, weights):
    return jnp.einsum("tf,df->td", hidden_rows, weights, preferred_element_type=jnp.float32)


def fold_rows(left, right):
    return jnp.einsum("ta,tb->ab", left, right, preferred_element_type=jnp.float32)


def own_rows(rows):
    count = rows.shape[0] // lax.axis_size("tp")
    return lax.dynamic_slice_in_dim(rows, lax.axis_index("tp") * count, count, axis=0)


def sum_rows(partial):
    shares = lax.all_to_all(
        partial.astype(jnp.bfloat16), "tp", split_axis=0, concat_axis=0, tiled=True
    )
    shares = shares.reshape((lax.axis_size("tp"), -1, shares.shape[1]))
    return jnp.sum(shares.astype(jnp.float32), axis=0)


def join_rows(rows):
    return lax.all_gather(rows, "tp", axis=0, tiled=True)


def block_forward(values, gain_vector, weights, width):
    widened, factor, normed = normalize(values, gain_vector)
    pre = project(normed, weights[:, : 2 * width])
    hidden = (jax.nn.silu(pre[:, :width]) * pre[:, width:]).astype(jnp.bfloat16)
    branch = sum_rows(project_back(hidden, weights[:, 2 * width :]))
    return join_rows((own_rows(widened) + 0.5 * branch).astype(jnp.bfloat16))


def block_backward(normalized, cotangent, weights, width):
    widened, factor, normed = normalized
    pre = project(normed, weights[:, : 2 * width])
    gate_pre, up_pre = pre[:, :width], pre[:, width:]
    sigmoid_gate = jax.nn.sigmoid(gate_pre)
    activated = gate_pre * sigmoid_gate
    hidden = (activated * up_pre).astype(jnp.bfloat16)
    hidden_grad = 0.5 * project(cotangent, weights[:, 2 * width :])
    gate_grad = (
        hidden_grad * up_pre * sigmoid_gate * (1.0 + gate_pre * (1.0 - sigmoid_gate))
    ).astype(jnp.bfloat16)
    up_grad = (hidden_grad * activated).astype(jnp.bfloat16)
    pieces = jnp.concatenate((gate_grad, up_grad, hidden), axis=1)
    partial_value = project_back(pieces[:, : 2 * width], weights[:, : 2 * width])
    return (partial_value, pieces)


def backward_rows(normalized, cotangent, gain_vector, partial_value):
    normed_grad = sum_rows(partial_value)
    widened, factor = own_rows(normalized[0]), own_rows(normalized[1])
    scaled = normed_grad * gain_vector
    unit_rows = widened * factor
    rows_grad = own_rows(cotangent).astype(jnp.float32) + factor * (
        scaled - unit_rows * jnp.mean(scaled * unit_rows, axis=-1, keepdims=True)
    )
    return rows_grad.astype(jnp.bfloat16)


def gather_weights(gate, up, down):
    return lax.all_gather(jnp.concatenate((gate, up, down.T), axis=1), "fs", axis=0, tiled=True)


def share_columns(rows):
    return lax.all_to_all(rows, "fs", split_axis=1, concat_axis=0, tiled=True)


def join_columns(share):
    joined = join_rows(share)
    parts = joined.reshape((lax.axis_size("tp"), lax.axis_size("fs"), -1, joined.shape[1]))
    return jnp.swapaxes(parts, 0, 1).reshape(joined.shape)


def per_device(
    late_input,
    early_input,
    early_mid,
    cotangent,
    gain_first,
    gain_second,
    gate_first,
    up_first,
    down_first,
    gate_second,
    up_second,
    down_second,
    sum_gate_first,
    sum_up_first,
    sum_down_first,
    sum_gate_second,
    sum_up_second,
    sum_down_second,
):
    width = gate_first.shape[1]
    weights_second = gather_weights(gate_second, up_second, down_second)
    weights_first = gather_weights(gate_first, up_first, down_first)
    norm_second = normalize(early_mid, gain_second)
    norm_first = normalize(early_input, gain_first)
    early_rows = jnp.stack(
        (own_rows(norm_second[2]), own_rows(norm_first[2]), own_rows(cotangent))
    )
    early_shares = lax.all_to_all(early_rows, "fs", split_axis=2, concat_axis=1, tiled=True)
    columns_second = join_columns(early_shares[0])
    columns_first = join_columns(early_shares[1])
    columns_cotangent = join_columns(early_shares[2])
    weights_second, columns_second, columns_first, columns_cotangent = lax.optimization_barrier(
        (weights_second, columns_second, columns_first, columns_cotangent)
    )

    partial_second, pieces_second = block_backward(
        norm_second, cotangent, weights_second, width
    )
    all_second = lax.all_gather(pieces_second, "fs", axis=0, tiled=True)
    mid_rows = backward_rows(norm_second, cotangent, gain_second, partial_second)
    mid_grad = join_rows(mid_rows)
    columns_mid = join_columns(share_columns(mid_rows))
    weights_first, pieces_second, mid_grad, columns_mid = lax.optimization_barrier(
        (weights_first, pieces_second, mid_grad, columns_mid)
    )
    partial_first, pieces_first = block_backward(norm_first, mid_grad, weights_first, width)
    all_first = lax.all_gather(pieces_first, "fs", axis=0, tiled=True)
    late_mid = block_forward(late_input, gain_first, weights_first, width)
    input_grad = join_rows(backward_rows(norm_first, mid_grad, gain_first, partial_first))
    late_out = block_forward(late_mid, gain_second, weights_second, width)
    all_second, late_out, input_grad = lax.optimization_barrier((all_second, late_out, input_grad))

    def collect(pieces, columns_in, columns_out, sums):
        return (
            sums[0] + fold_rows(columns_in, pieces[:, :width]),
            sums[1] + fold_rows(columns_in, pieces[:, width : 2 * width]),
            sums[2] + 0.5 * fold_rows(pieces[:, 2 * width :], columns_out),
        )

    new_second = collect(
        all_second, columns_second, columns_cotangent, (sum_gate_second, sum_up_second, sum_down_second)
    )
    all_first, new_second = lax.optimization_barrier((all_first, new_second))
    new_first = collect(
        all_first, columns_first, columns_mid, (sum_gate_first, sum_up_first, sum_down_first)
    )
    return (late_mid, late_out, input_grad) + new_first + new_second


def solution(mesh):
    in_specs = (
        P("fs", None),
        P("fs", None),
        P("fs", None),
        P("fs", None),
        P(),
        P(),
        P("fs", "tp"),
        P("fs", "tp"),
        P("tp", "fs"),
        P("fs", "tp"),
        P("fs", "tp"),
        P("tp", "fs"),
        P("fs", "tp"),
        P("fs", "tp"),
        P("tp", "fs"),
        P("fs", "tp"),
        P("fs", "tp"),
        P("tp", "fs"),
    )
    out_specs = (
        P("fs", None),
        P("fs", None),
        P("fs", None),
        P("fs", "tp"),
        P("fs", "tp"),
        P("tp", "fs"),
        P("fs", "tp"),
        P("fs", "tp"),
        P("tp", "fs"),
    )
    return jax.shard_map(
        per_device, mesh=mesh, in_specs=in_specs, out_specs=out_specs, check_vma=False
    )
```
